32 devices in a mesh: sp: 4 (over z), tp: 8 (over y, x, core).
Axes of the slice: x: 2, y: 2, z: 4, core: 2. Of those that a mesh axis runs over, the one named last changes fastest.
Arguments:
- tokens: bfloat16 [1536, 2048], P('sp', 'tp'), may hold values from -6 to 6
- norm_gain: bfloat16 [2048], replicated, may hold values from 0.099609375 to 1.8984375
- lin_query: bfloat16 [2048, 1024], P(None, 'tp'), may hold values from -0.125 to 0.125
- lin_key: bfloat16 [2048, 1024], P(None, 'tp'), may hold values from -0.125 to 0.125
- lin_value: bfloat16 [2048, 1024], P(None, 'tp'), may hold values from -0.125 to 0.125
- lin_gate: bfloat16 [2048, 1024], P(None, 'tp'), may hold values from -0.125 to 0.125
- gate_down: bfloat16 [2048, 32], replicated, may hold values from -0.125 to 0.125
- gate_up_weight: bfloat16 [32, 1024], replicated, may hold values from -1 to 1
- decay_offset_bias: float32 [1536, 1024], P('sp', 'tp'), may hold values from -16 to 11
- lin_norm_gain: float32 [128], replicated, may hold values from 0.1 to 1.9
- stick_query: bfloat16 [2048, 1024], P(None, 'tp'), may hold values from -0.25 to 0.25
- stick_key: bfloat16 [2048, 1024], P(None, 'tp'), may hold values from -0.25 to 0.25
- stick_value: bfloat16 [2048, 1024], P(None, 'tp'), may hold values from -0.125 to 0.125
- key_bias: bfloat16 [8, 1536], P('tp', 'sp'), may hold values from -20 to -2
- out_linear: bfloat16 [1024, 2048], replicated, may hold values from -0.125 to 0.125
- out_stick: bfloat16 [1024, 2048], replicated, may hold values from -0.125 to 0.125
Outputs:
- mixed: bfloat16 [1536, 2048], P(('sp', 'tp'))
The draws below stay inside these ranges and needn't reach their ends.
All inputs are finite; a program needn't handle non-finite values.
Results may differ from the reference program's by a relative error of at most 0.012.
Values may be sent and summed in bfloat16 or wider, within the bound.
No kernel may reach another device: no remote copies, remote signals or barrier semaphores. Data moves between devices by JAX's collectives and lax.ppermute only.
A program may use at most 64 MiB of HBM per device.

```python
import math
import jax
import jax.numpy as jnp
from jax import lax

D = 2048
GH = 8
HS = 8
DK = 128
RANK = 32
BLK = 32
TOK_DEV = 384
SEQUENCE_LENGTH = 1536


def segment_rows(key_segment):
    position_index = jax.random.randint(key_segment, (4,), 0, SEQUENCE_LENGTH)
    return jnp.any(jnp.arange(SEQUENCE_LENGTH)[:, None] == position_index[None, :], axis=1)


def draw_decay_offset_bias(key, part):
    key_rows = jax.random.split(jax.random.fold_in(key, 11), 5)
    slow_heads = jax.random.randint(key_rows[0], (GH,), 0, 2) > 0
    span_count = SEQUENCE_LENGTH // TOK_DEV
    offsets = jax.random.uniform(key_rows[1], (span_count, GH), jnp.float32, -0.7, 0.7)
    span_of = jnp.arange(SEQUENCE_LENGTH) // TOK_DEV
    fast_level = jax.random.uniform(key_rows[2], (GH,), jnp.float32, -0.5, 1.5)
    level = jnp.where(slow_heads, 9.5, fast_level)
    head_wise = level[None, :] + offsets[span_of]
    random_jitter = jax.random.uniform(key_rows[3], (SEQUENCE_LENGTH, GH, DK), jnp.float32, -0.5, 0.5)
    segment_list = segment_rows(key_rows[4]).astype(jnp.float32)
    value_rows = head_wise[:, :, None] + random_jitter - 14.0 * segment_list[:, None, None]
    return value_rows.reshape(SEQUENCE_LENGTH, GH * DK)


def draw_key_bias(key, part):
    key_rows = jax.random.split(jax.random.fold_in(key, 23), 5)
    slow_heads = jax.random.randint(key_rows[0], (HS,), 0, 2) > 0
    span_count = SEQUENCE_LENGTH // TOK_DEV
    offsets = jax.random.uniform(key_rows[1], (HS, span_count), jnp.float32, -0.7, 0.7)
    span_of = jnp.arange(SEQUENCE_LENGTH) // TOK_DEV
    fast_level = jax.random.uniform(key_rows[2], (HS,), jnp.float32, -12.5, -11.5)
    level = jnp.where(slow_heads, -8.0 - math.log(SEQUENCE_LENGTH), fast_level)
    head_wise = level[:, None] + offsets[:, span_of]
    random_jitter = jax.random.uniform(key_rows[3], (HS, SEQUENCE_LENGTH), jnp.float32, -0.5, 0.5)
    segment_list = segment_rows(key_rows[4]).astype(jnp.float32)
    value_rows = head_wise + random_jitter + 8.0 * segment_list[None, :]
    return value_rows.astype(jnp.bfloat16)


def shard_levels(rng, extent, pieces, low, largest):
    factor_of = 1.0
    for axis_at, blocks in pieces:
        draws = jax.random.uniform(jax.random.fold_in(jax.random.fold_in(rng, 6), axis_at), (blocks,), jnp.float32, low / len(pieces), largest / len(pieces))
        factor_of = factor_of * jnp.repeat(jnp.exp(draws), extent[axis_at] // blocks).reshape((-1,) + (1,) * (len(extent) - 1 - axis_at))
    return factor_of


def noise(stream_key, shape, scale, bound, pieces=(), held_as=jnp.bfloat16):
    factor_of = shard_levels(stream_key, shape, pieces, -0.22, 0.18) if pieces else 1.0
    values = jax.random.normal(stream_key, shape, jnp.float32) * scale * factor_of
    return jnp.minimum(jnp.maximum(values, -bound), bound).astype(held_as)


def setup_inputs(seed: int = 0) -> dict:
    splits = jax.random.split(jax.random.key(seed), 17)
    tokens = noise(splits[0], (SEQUENCE_LENGTH, D), 1.0, 6.0, ((0, 4), (1, 8)))
    norm_gain = jnp.clip(1.0 + 0.18 * jax.random.normal(splits[1], (D,), jnp.float32), 0.099609375, 1.8984375).astype(jnp.bfloat16)
    lin_query = noise(splits[2], (D, GH * DK), D ** -0.5, 0.125, ((1, 8),))
    lin_key = noise(splits[3], (D, GH * DK), D ** -0.5, 0.125, ((1, 8),))
    lin_value = noise(splits[4], (D, GH * DK), D ** -0.5, 0.125, ((1, 8),))
    lin_gate = noise(splits[5], (D, GH * DK), D ** -0.5, 0.125, ((1, 8),))
    gate_down = noise(splits[6], (D, RANK), D ** -0.5, 0.125)
    gate_up_weight = noise(splits[7], (RANK, GH * DK), RANK ** -0.5, 1.0)
    decay_offset_bias = draw_decay_offset_bias(jax.random.fold_in(splits[16], 71), 0)
    lin_norm_gain = jnp.clip(1.0 + 0.18 * jax.random.normal(splits[9], (DK,), jnp.float32), 0.1, 1.9)
    stick_query = noise(splits[10], (D, HS * DK), (D // 4) ** -0.5, 0.25, ((1, 8),))
    stick_key = noise(splits[11], (D, HS * DK), (D // 4) ** -0.5, 0.25, ((1, 8),))
    stick_value = noise(splits[12], (D, HS * DK), D ** -0.5, 0.125, ((1, 8),))
    key_bias = draw_key_bias(jax.random.fold_in(splits[16], 71), 0)
    out_linear = noise(splits[14], (GH * DK, D), (GH * DK + HS * DK) ** -0.5, 0.125)
    out_stick = noise(splits[15], (HS * DK, D), (GH * DK + HS * DK) ** -0.5, 0.125)
    return {"tokens": tokens, "norm_gain": norm_gain, "lin_query": lin_query, "lin_key": lin_key, "lin_value": lin_value, "lin_gate": lin_gate, "gate_down": gate_down, "gate_up_weight": gate_up_weight, "decay_offset_bias": decay_offset_bias, "lin_norm_gain": lin_norm_gain, "stick_query": stick_query, "stick_key": stick_key, "stick_value": stick_value, "key_bias": key_bias, "out_linear": out_linear, "out_stick": out_stick}


norm_eps = 1e-06
gate_softness = 16.0

def linear_attention(queries, keys_in, values_in, decay_logarithm, gate_in, head_gain):
    blocks = SEQUENCE_LENGTH // BLK
    highest_precision = lax.Precision.HIGHEST

    def blocked(matrix):
        return matrix.reshape(blocks, BLK, GH, DK).transpose(0, 2, 1, 3)
    causal = jnp.tril(jnp.ones((BLK, BLK), dtype=bool))

    def advance(running_state, inputs):
        query_block, key_block, value_block, decay_blk = inputs
        within_segment = jnp.cumsum(decay_blk, axis=1)
        carried_state = jnp.einsum('cgw,cwz->cgz', query_block * jnp.exp(within_segment), running_state, precision=highest_precision)
        spread = within_segment[:, :, None, :] - within_segment[:, None, :, :]
        fading = jnp.exp(jnp.where(causal[:, :, None], spread, -jnp.inf))
        scores = jnp.einsum('htk,hsk,htsk->hts', query_block, key_block, fading, precision=highest_precision)
        rounded = lax.optimization_barrier(scores.astype(jnp.bfloat16))
        inner = jnp.einsum('hts,hsv->htv', rounded.astype(jnp.float32), value_block.astype(jnp.float32), precision=highest_precision)
        last_position = within_segment[:, -1, :]
        fresh_state = jnp.einsum('iga,igl->ial', key_block * jnp.exp(last_position[:, None, :] - within_segment), value_block.astype(jnp.float32), precision=highest_precision)
        new_state = running_state * jnp.exp(last_position)[:, :, None] + fresh_state
        return (new_state, carried_state + inner)
    scaled_queries = blocked(queries).astype(jnp.float32) * DK ** (-0.5)
    start_state = jnp.zeros((GH, DK, DK), jnp.float32)
    _, outputs = lax.scan(advance, start_state, (scaled_queries, blocked(keys_in).astype(jnp.float32), blocked(values_in), blocked(decay_logarithm)))
    combined = outputs.transpose(0, 2, 1, 3).reshape(SEQUENCE_LENGTH, GH, DK)
    normed = combined * lax.rsqrt(lax.optimization_barrier(jnp.mean(combined * combined, axis=-1, keepdims=True)) + norm_eps) * head_gain
    return (normed.reshape(SEQUENCE_LENGTH, GH * DK) * jax.nn.silu(gate_in.astype(jnp.float32))).astype(jnp.bfloat16)

def stick_attention(queries, keys_in, values_in, key_bias):
    span_count = SEQUENCE_LENGTH // TOK_DEV
    key_pos = jnp.arange(SEQUENCE_LENGTH, dtype=jnp.int32)

    def head_wise(matrix):
        return matrix.reshape(SEQUENCE_LENGTH, HS, DK).transpose(1, 0, 2)

    def one_head(inputs):
        head_query, head_key, head_value, head_bias = inputs
        starts = jnp.arange(span_count, dtype=jnp.int32) * TOK_DEV

        def one_span(span_in):
            span_query, first = span_in
            logits = jnp.dot(span_query, head_key.T, preferred_element_type=jnp.float32) * DK ** (-0.5) + head_bias.astype(jnp.float32)[None, :]
            query_pos = first + jnp.arange(TOK_DEV, dtype=jnp.int32)
            visible = key_pos[None, :] < query_pos[:, None]
            falling = jnp.where(visible, jax.nn.log_sigmoid(-logits), 0.0)
            behind = lax.cumsum(falling, axis=1, reverse=True) - falling
            shares = jnp.where(visible, jnp.exp(jax.nn.log_sigmoid(logits) + behind), 0.0).astype(jnp.bfloat16)
            return jnp.dot(shares, head_value, preferred_element_type=jnp.float32)
        spans = lax.map(one_span, (head_query.reshape(span_count, TOK_DEV, DK), starts))
        return spans.reshape(SEQUENCE_LENGTH, DK)
    heads_out = lax.map(one_head, (head_wise(queries), head_wise(keys_in), head_wise(values_in), key_bias))
    return heads_out.transpose(1, 0, 2).reshape(SEQUENCE_LENGTH, HS * DK).astype(jnp.bfloat16)

def reference(tokens, norm_gain, lin_query, lin_key, lin_value, lin_gate, gate_down, gate_up_weight, decay_offset_bias, lin_norm_gain, stick_query, stick_key, stick_value, key_bias, out_linear, out_stick):
    widened = tokens.astype(jnp.float32)
    inv_rms = lax.rsqrt(lax.optimization_barrier(jnp.mean(widened * widened, axis=1)) + norm_eps)[:, None]
    scaled = (widened * norm_gain.astype(jnp.float32)).astype(jnp.bfloat16)

    def project(weight):
        return (jnp.dot(scaled, weight, preferred_element_type=jnp.float32) * inv_rms).astype(jnp.bfloat16)
    reduced_rank = project(gate_down)
    decay_logarithm = jax.nn.log_sigmoid(jnp.dot(reduced_rank, gate_up_weight, preferred_element_type=jnp.float32) + decay_offset_bias) / gate_softness
    linear_out = linear_attention(project(lin_query), project(lin_key), project(lin_value), decay_logarithm, project(lin_gate), lin_norm_gain)
    stick_out = stick_attention(project(stick_query), project(stick_key), project(stick_value), key_bias)
    total = jnp.dot(linear_out, out_linear, preferred_element_type=jnp.float32) + jnp.dot(stick_out, out_stick, preferred_element_type=jnp.float32)
    return total.astype(jnp.bfloat16)
```

```python
import functools
import math

import jax
import jax.numpy as jnp
import numpy as np
from jax import lax
from jax.experimental import pallas as pl
from jax.experimental.pallas import tpu as pltpu
from jax.sharding import PartitionSpec as P


norm_eps = 1e-06
gate_softness = 16.0
CHUNK = 128
PAD = 16
f32 = jnp.float32
bf16 = jnp.bfloat16
VMEM = pl.BlockSpec(memory_space=pltpu.VMEM)
SMEM = pl.BlockSpec(memory_space=pltpu.SMEM)


def dot(a, b):
    return jnp.dot(a, b, preferred_element_type=f32)


def dot_nt(a, b):
    return lax.dot_general(a, b, (((1,), (1,)), ((), ())), preferred_element_type=f32)


def dot_tn(a, b):
    return lax.dot_general(a, b, (((0,), (0,)), ((), ())), preferred_element_type=f32)


def split(x):
    hi = x.astype(bf16)
    return hi, (x - hi.astype(f32)).astype(bf16)


def halvings():
    size, result = CHUNK // 2, []
    while size:
        result.append(size)
        size //= 2
    return result


def span_matrices():
    t, i = np.arange(CHUNK)[:, None], np.arange(CHUNK)[None, :]
    parts = []
    for h in halvings():
        pivot = (t // (2 * h)) * 2 * h + h - 1
        parts.append(np.where(t > pivot, (i > pivot) & (i <= t), (i > t) & (i <= pivot)))
    parts.append(i <= t)
    parts.append(i > t)
    return np.concatenate(parts, 0).astype(np.float32)


def project_first(*refs, halves):
    tokens, (gain, wk, wv, bias, scaled, rescale, pack) = refs[:halves], refs[halves:]
    pieces, rows, width = tokens[0].shape
    count = rows * halves
    for a in range(halves):
        squares = jnp.zeros((rows, 1), f32)
        for j in range(pieces):
            part = tokens[a][j].astype(f32)
            squares = squares + jnp.sum(part * part, axis=1, keepdims=True)
            g = gain[:, j * width : (j + 1) * width].astype(f32)
            scaled[a * rows : (a + 1) * rows, j * width : (j + 1) * width] = (part * g).astype(bf16)
        rescale[a * rows : (a + 1) * rows, :] = lax.rsqrt(squares / (pieces * width) + norm_eps)
    both = dot(scaled[...], jnp.concatenate([wk[...], wv[...]], axis=1)) * rescale[...]
    cols = wk.shape[1]
    pack[:count, :] = both[:, :cols].astype(bf16)
    pack[count : 2 * count, :] = both[:, cols:].astype(bf16)
    extra = pack.shape[0] - 2 * count
    heads = bias.shape[0]
    head_size = cols // heads
    row = lax.broadcasted_iota(jnp.int32, (extra, head_size), 0)
    for h in range(heads):
        block = jnp.zeros((extra, head_size), f32)
        for m in range(count // head_size):
            piece = bias[h : h + 1, m * head_size : (m + 1) * head_size].astype(f32)
            block = jnp.where(row == m, piece, block)
        pack[2 * count :, h * head_size : (h + 1) * head_size] = block.astype(bf16)


def stick_block(query, pack, acc, consumed, head, head_size, own):
    count = query.shape[0]
    cols = pl.ds(head * head_size, head_size)
    j = lax.broadcasted_iota(jnp.int32, (2 * CHUNK, CHUNK), 0) % CHUNK
    s = lax.broadcasted_iota(jnp.int32, (2 * CHUNK, CHUNK), 1)
    later = (j >= s).astype(bf16)
    for m in reversed(range(count // CHUNK)):
        first = m * CHUNK if own else 0
        rows = pl.ds(first, count - first)
        keys = pack[pl.ds(m * CHUNK, CHUNK), cols]
        values = pack[pl.ds(count + m * CHUNK, CHUNK), cols]
        bias = pack[pl.ds(2 * count, PAD), cols][m : m + 1, :].astype(f32)
        z = dot_nt(query[rows, cols], keys) * head_size ** (-0.5) + bias
        falling = -(jnp.maximum(z, 0.0) + jnp.log(1.0 + jnp.exp(-jnp.abs(z))))
        if own:
            t = lax.broadcasted_iota(jnp.int32, z.shape, 0)
            visible = lax.broadcasted_iota(jnp.int32, z.shape, 1) < t
            falling = jnp.where(visible, falling, 0.0)
        sums = dot(jnp.concatenate(split(falling), axis=1), later)
        before = consumed[rows, pl.ds(head, 1)]
        shares = jnp.exp(z + sums + before)
        if own:
            shares = jnp.where(visible, shares, 0.0)
        acc[rows, cols] += dot(shares.astype(bf16), values)
        consumed[rows, pl.ds(head, 1)] = before + sums[:, 0:1]


def project_rest(
    scaled, rescale, wsq, wq, wk, wv, wg, down, up, bias, pack, spans,
    local_out, from_start, gate, summary, sq, acc, consumed,
):
    cols = wq.shape[1]
    head_size = CHUNK
    count = scaled.shape[0]
    scale = head_size ** (-0.5)
    inv = rescale[...]
    x = scaled[...]
    low = (dot(x, down[...]) * inv).astype(bf16)
    pre = dot(low, up[...]) + bias[...]
    decay = (jnp.minimum(pre, 0.0) - jnp.log(1.0 + jnp.exp(-jnp.abs(pre)))) / gate_softness
    qk = dot(x, jnp.concatenate([wq[...], wk[...]], axis=1)) * inv
    vg = dot(x, jnp.concatenate([wv[...], wg[...]], axis=1)) * inv
    gate[...] = vg[:, cols:].astype(bf16)
    sq[...] = (dot(x, wsq[...]) * inv).astype(bf16)
    t = lax.broadcasted_iota(jnp.int32, (CHUNK, CHUNK), 0)
    s = lax.broadcasted_iota(jnp.int32, (CHUNK, CHUNK), 1)
    sizes = halvings()
    for h in range(cols // head_size):
        at = slice(h * head_size, (h + 1) * head_size)
        state = jnp.zeros((head_size, head_size), f32)
        offset = jnp.zeros((1, head_size), f32)
        for n in range(count // CHUNK):
            rows = slice(n * CHUNK, (n + 1) * CHUNK)
            q16 = qk[rows, h * head_size : (h + 1) * head_size].astype(bf16)
            k16 = qk[rows, cols + h * head_size : cols + (h + 1) * head_size].astype(bf16)
            v16 = vg[rows, at].astype(bf16)
            q, k = q16.astype(f32), k16.astype(f32)
            both = dot(spans[...], jnp.concatenate(split(decay[rows, at]), axis=1))
            exponents = both[:, :head_size] + both[:, head_size:]
            scores = jnp.where(t == s, dot_nt(q16, k16), 0.0)
            for level, size in enumerate(sizes):
                e = jnp.exp(exponents[level * CHUNK : (level + 1) * CHUNK])
                part = dot_nt((q * e).astype(bf16), (k * e).astype(bf16))
                ok = (t // (2 * size) == s // (2 * size)) & (t % (2 * size) >= size)
                scores = jnp.where(ok & (s % (2 * size) < size), part, scores)
            since = exponents[len(sizes) * CHUNK : (len(sizes) + 1) * CHUNK]
            until = exponents[(len(sizes) + 1) * CHUNK :]
            inner = dot((scores * scale).astype(bf16), v16)
            carried = dot_nt((q * scale * jnp.exp(since)).astype(bf16), state.astype(bf16))
            local_out[rows, at] = inner + carried
            from_start[rows, at] = (q * scale * jnp.exp(since + offset)).astype(bf16)
            total = since[CHUNK - 1 : CHUNK, :]
            state = state * jnp.exp(total) + dot_tn(v16, (k * jnp.exp(until)).astype(bf16))
            offset = offset + total
        summary[:head_size, at] = state.astype(bf16)
        row = lax.broadcasted_iota(jnp.int32, (PAD, head_size), 0)
        high, rest = split(offset)
        tail = jnp.where(row == 0, high.astype(f32), jnp.where(row == 1, rest.astype(f32), 0.0))
        summary[head_size:, at] = tail.astype(bf16)
    acc[...] = jnp.zeros_like(acc)
    consumed[...] = jnp.zeros_like(consumed)
    for h in range(sq.shape[1] // head_size):
        stick_block(sq, pack, acc, consumed, h, head_size, True)


def finish(*refs, steps):
    position, local_out, from_start, gate, head_gain, sq, acc_in, consumed_in = refs[:8]
    packs, summaries = refs[8 : 8 + steps], refs[8 + steps : 8 + 2 * steps]
    merged, acc, consumed, state = refs[8 + 2 * steps :]
    head_size = head_gain.shape[1]
    here = position[0]
    acc[...] = acc_in[...]
    consumed[...] = consumed_in[...]
    state[...] = jnp.zeros_like(state)
    for r in range(1, steps + 1):

        @pl.when(r <= here)
        def _(pack=packs[r - 1]):
            for h in range(sq.shape[1] // head_size):
                stick_block(sq, pack, acc, consumed, h, head_size, False)

    for r in range(steps, 0, -1):

        @pl.when(r <= here)
        def _(one=summaries[r - 1]):
            tail = one[head_size:, :].astype(f32)
            kept = jnp.exp(tail[0:1, :] + tail[1:2, :])
            state[...] = state[...] * kept + one[:head_size, :].astype(f32)

    lin_cols = local_out.shape[1]
    for h in range(lin_cols // head_size):
        at = slice(h * head_size, (h + 1) * head_size)
        out = local_out[:, at] + dot_nt(from_start[:, at], state[:, at].astype(bf16))
        out = out * lax.rsqrt(jnp.mean(out * out, axis=1, keepdims=True) + norm_eps) * head_gain[...]
        g = gate[:, at].astype(f32)
        merged[:, at] = (out * (g / (1.0 + jnp.exp(-g)))).astype(bf16)
    merged[:, lin_cols:] = acc[...].astype(bf16)


def call(body, outs, count, scratch=(), flops=0, name=None):
    return pl.pallas_call(
        body,
        out_shape=outs,
        in_specs=count,
        out_specs=[VMEM] * len(outs),
        scratch_shapes=scratch,
        cost_estimate=pl.CostEstimate(flops=flops, bytes_accessed=1 << 22, transcendentals=1 << 20),
        name=name,
    )


def sent_back(array, axis):
    devices, here = lax.axis_size(axis), lax.axis_index(axis)
    if devices <= 8:
        return [
            lax.ppermute(array, axis, [(i, i + r) for i in range(devices - r)])
            for r in range(1, devices)
        ]
    everything = lax.all_gather(array, axis)
    return [
        lax.dynamic_index_in_dim(everything, (here - r) % devices, 0, keepdims=False)
        for r in range(1, devices)
    ]


def gathered(tokens):
    members = lax.axis_size("tp")
    total = tokens.size * members * tokens.dtype.itemsize
    halves = 1
    while total // halves >= 1 << 20:
        halves *= 2
    rows = tokens.shape[0] // halves
    result, rest = [], tokens
    for a in range(halves):
        result.append(lax.all_gather(rest[a * rows : (a + 1) * rows], "tp"))
        result[-1], rest = lax.optimization_barrier((result[-1], rest))
    return result


def per_device(
    tokens, norm_gain, lin_query, lin_key, lin_value, lin_gate, gate_down, gate_up_weight,
    decay_offset_bias, lin_norm_gain, stick_query, stick_key, stick_value, key_bias,
    out_linear, out_stick,
):
    model_width = norm_gain.shape[0]
    head_size = lin_norm_gain.shape[0]
    count = tokens.shape[0]
    lin_cols, stick_cols = lin_query.shape[1], stick_query.shape[1]
    stick_heads = stick_cols // head_size
    shape = jax.ShapeDtypeStruct
    parts = gathered(tokens)
    scaled, rescale, pack = call(
        functools.partial(project_first, halves=len(parts)),
        [shape((count, model_width), bf16), shape((count, 1), f32),
         shape((2 * count + PAD, stick_cols), bf16)],
        [VMEM] * (len(parts) + 4), flops=4 * count * model_width * stick_cols, name="first",
    )(*parts, norm_gain[None], stick_key, stick_value, key_bias)
    packs = sent_back(pack, "sp")
    up = lax.dynamic_slice_in_dim(gate_up_weight, lax.axis_index("tp") * lin_cols, lin_cols, 1)
    local_out, from_start, gate, summary, sq, acc, consumed = call(
        project_rest,
        [shape((count, lin_cols), f32), shape((count, lin_cols), bf16),
         shape((count, lin_cols), bf16), shape((head_size + PAD, lin_cols), bf16),
         shape((count, stick_cols), bf16), shape((count, stick_cols), f32),
         shape((count, stick_heads), f32)],
        [VMEM] * 12, flops=1 << 34, name="rest",
    )(scaled, rescale, stick_query, lin_query, lin_key, lin_value, lin_gate, gate_down, up,
      decay_offset_bias, pack, jnp.asarray(span_matrices(), bf16))
    summaries = sent_back(summary, "sp")
    steps = len(packs)
    (merged,) = call(
        functools.partial(finish, steps=steps),
        [shape((count, lin_cols + stick_cols), bf16)],
        [SMEM] + [VMEM] * (7 + 2 * steps),
        scratch=[pltpu.VMEM((count, stick_cols), f32), pltpu.VMEM((count, stick_heads), f32),
                 pltpu.VMEM((head_size, lin_cols), f32)],
        flops=1 << 32, name="finish",
    )(lax.axis_index("sp")[None].astype(jnp.int32), local_out, from_start, gate,
      lin_norm_gain[None], sq, acc, consumed, *packs, *summaries)
    members = lax.axis_size("tp")
    joined = lin_cols + stick_cols
    received = lax.all_to_all(
        merged.reshape(members, count // members, joined), "tp", split_axis=0, concat_axis=0, tiled=True
    )
    lin_part = jnp.concatenate([received[j, :, :lin_cols] for j in range(members)], axis=1)
    stick_part = jnp.concatenate([received[j, :, lin_cols:] for j in range(members)], axis=1)
    total = dot(lin_part, out_linear) + dot(stick_part, out_stick)
    return total.astype(bf16)


def solution(mesh):
    heads = P(None, "tp")
    placed = (
        P("sp", "tp"), P(), heads, heads, heads, heads, P(), P(), P("sp", "tp"), P(),
        heads, heads, heads, P("tp", "sp"), P(), P(),
    )
    return jax.shard_map(
        per_device, mesh=mesh, in_specs=placed, out_specs=P(("sp", "tp"), None), check_vma=False
    )
```

```python
import functools

import jax
import jax.numpy as jnp
import numpy as np
from jax import lax
from jax.experimental import pallas as pl
from jax.experimental.pallas import tpu as pltpu
from jax.sharding import PartitionSpec as P


norm_eps = 1e-06
gate_softness = 16.0
CHUNK = 128
PAD = 16
f32 = jnp.float32
bf16 = jnp.bfloat16
VMEM = pl.BlockSpec(memory_space=pltpu.VMEM)
SMEM = pl.BlockSpec(memory_space=pltpu.SMEM)


def dot(a, b):
    return jnp.dot(a, b, preferred_element_type=f32)


def dot_nt(a, b):
    return lax.dot_general(a, b, (((1,), (1,)), ((), ())), preferred_element_type=f32)


def dot_tn(a, b):
    return lax.dot_general(a, b, (((0,), (0,)), ((), ())), preferred_element_type=f32)


def split(x):
    hi = x.astype(bf16)
    return hi, (x - hi.astype(f32)).astype(bf16)


def halvings():
    size, result = CHUNK // 2, []
    while size:
        result.append(size)
        size //= 2
    return result


def span_matrices():
    t, i = np.arange(CHUNK)[:, None], np.arange(CHUNK)[None, :]
    parts = []
    for h in halvings():
        pivot = (t // (2 * h)) * 2 * h + h - 1
        parts.append(np.where(t > pivot, (i > pivot) & (i <= t), (i > t) & (i <= pivot)))
    parts.append(i <= t)
    parts.append(i > t)
    return np.concatenate(parts, 0).astype(np.float32)


def project_first(core, same, other, gain, wk, wv, bias, scaled, rescale, pack, wide_gain):
    pieces, count, width = same.shape
    wide_gain[...] = gain[...].astype(f32)[None]
    squares = jnp.zeros((count, 1), f32)
    for tokens, parity in ((same, core[0]), (other, 1 - core[0])):
        for j in range(pieces):
            at = pl.ds(pl.multiple_of((2 * j + parity) * width, CHUNK), width)
            part = tokens[j].astype(f32)
            squares = squares + jnp.sum(part * part, axis=1, keepdims=True)
            scaled[:, at] = (part * wide_gain[:, at]).astype(bf16)
    rescale[...] = lax.rsqrt(squares / scaled.shape[1] + norm_eps)
    both = dot(scaled[...], jnp.concatenate([wk[...], wv[...]], axis=1)) * rescale[...]
    cols = wk.shape[1]
    pack[:count, :] = both[:, :cols].astype(bf16)
    pack[count : 2 * count, :] = both[:, cols:].astype(bf16)
    extra = pack.shape[0] - 2 * count
    heads = bias.shape[0]
    head_size = cols // heads
    row = lax.broadcasted_iota(jnp.int32, (extra, head_size), 0)
    for h in range(heads):
        block = jnp.zeros((extra, head_size), f32)
        for m in range(count // head_size):
            piece = bias[h : h + 1, m * head_size : (m + 1) * head_size].astype(f32)
            block = jnp.where(row == m, piece, block)
        pack[2 * count :, h * head_size : (h + 1) * head_size] = block.astype(bf16)


def stick_block(query, pack, acc, consumed, head, head_size, own):
    count = query.shape[0]
    cols = pl.ds(head * head_size, head_size)
    j = lax.broadcasted_iota(jnp.int32, (2 * CHUNK, CHUNK), 0) % CHUNK
    s = lax.broadcasted_iota(jnp.int32, (2 * CHUNK, CHUNK), 1)
    later = (j >= s).astype(bf16)
    for m in reversed(range(count // CHUNK)):
        first = m * CHUNK if own else 0
        rows = pl.ds(first, count - first)
        keys = pack[pl.ds(m * CHUNK, CHUNK), cols]
        values = pack[pl.ds(count + m * CHUNK, CHUNK), cols]
        bias = pack[pl.ds(2 * count, PAD), cols][m : m + 1, :].astype(f32)
        z = dot_nt(query[rows, cols], keys) * head_size ** (-0.5) + bias
        falling = -(jnp.maximum(z, 0.0) + jnp.log(1.0 + jnp.exp(-jnp.abs(z))))
        if own:
            t = lax.broadcasted_iota(jnp.int32, z.shape, 0)
            visible = lax.broadcasted_iota(jnp.int32, z.shape, 1) < t
            falling = jnp.where(visible, falling, 0.0)
        sums = dot(jnp.concatenate(split(falling), axis=1), later)
        before = consumed[rows, pl.ds(head, 1)]
        shares = jnp.exp(z + sums + before)
        if own:
            shares = jnp.where(visible, shares, 0.0)
        acc[rows, cols] += dot(shares.astype(bf16), values)
        consumed[rows, pl.ds(head, 1)] = before + sums[:, 0:1]


def decay_state(
    place, scaled, rescale, wk, wv, down, up, bias, spans, exponents, keys, values, summary,
):
    cols = wk.shape[1]
    head_size = CHUNK
    inv = rescale[...]
    x = scaled[...]
    low = (dot_nt(x, down[...]) * inv).astype(bf16)
    own = pl.ds(pl.multiple_of(place[0] * cols, CHUNK), cols)
    pre = dot(low, up[:, own]) + bias[...]
    decay = (jnp.minimum(pre, 0.0) - jnp.log(1.0 + jnp.exp(-jnp.abs(pre)))) / gate_softness
    kv = dot(x, jnp.concatenate([wk[...], wv[...]], axis=1)) * inv
    keys[...] = kv[:, :cols].astype(bf16)
    values[...] = kv[:, cols:].astype(bf16)
    size = spans.shape[0]
    for h in range(cols // head_size):
        at = slice(h * head_size, (h + 1) * head_size)
        state = jnp.zeros((head_size, head_size), f32)
        offset = jnp.zeros((1, head_size), f32)
        for n in range(x.shape[0] // CHUNK):
            rows = slice(n * CHUNK, (n + 1) * CHUNK)
            both = dot(spans[...], jnp.concatenate(split(decay[rows, at]), axis=1))
            both = both[:, :head_size] + both[:, head_size:]
            exponents[n * size : (n + 1) * size, at] = both
            until = both[size - CHUNK :]
            total = both[size - CHUNK - 1 : size - CHUNK, :]
            k = keys[rows, at].astype(f32)
            state = state * jnp.exp(total) + dot_tn(values[rows, at], (k * jnp.exp(until)).astype(bf16))
            offset = offset + total
        summary[:head_size, at] = state.astype(bf16)
        row = lax.broadcasted_iota(jnp.int32, (PAD, head_size), 0)
        high, rest = split(offset)
        tail = jnp.where(row == 0, high.astype(f32), jnp.where(row == 1, rest.astype(f32), 0.0))
        summary[head_size:, at] = tail.astype(bf16)


def project_rest(
    scaled, rescale, wsq, wq, wg, exponents_in, keys, values, pack,
    local_out, from_start, gate, sq, acc, consumed,
):
    cols = wq.shape[1]
    head_size = CHUNK
    count = scaled.shape[0]
    scale = head_size ** (-0.5)
    inv = rescale[...]
    x = scaled[...]
    qg = dot(x, jnp.concatenate([wq[...], wg[...]], axis=1)) * inv
    gate[...] = qg[:, cols:].astype(bf16)
    sq[...] = (dot(x, wsq[...]) * inv).astype(bf16)
    t = lax.broadcasted_iota(jnp.int32, (CHUNK, CHUNK), 0)
    s = lax.broadcasted_iota(jnp.int32, (CHUNK, CHUNK), 1)
    sizes = halvings()
    rows_each = exponents_in.shape[0] * CHUNK // count
    for h in range(cols // head_size):
        at = slice(h * head_size, (h + 1) * head_size)
        state = jnp.zeros((head_size, head_size), f32)
        offset = jnp.zeros((1, head_size), f32)
        for n in range(count // CHUNK):
            rows = slice(n * CHUNK, (n + 1) * CHUNK)
            q16 = qg[rows, at].astype(bf16)
            k16, v16 = keys[rows, at], values[rows, at]
            q, k = q16.astype(f32), k16.astype(f32)
            base = n * rows_each
            scores = jnp.where(t == s, dot_nt(q16, k16), 0.0)
            for level, size in enumerate(sizes):
                e = jnp.exp(exponents_in[base + level * CHUNK : base + (level + 1) * CHUNK, at])
                part = dot_nt((q * e).astype(bf16), (k * e).astype(bf16))
                ok = (t // (2 * size) == s // (2 * size)) & (t % (2 * size) >= size)
                scores = jnp.where(ok & (s % (2 * size) < size), part, scores)
            base = base + len(sizes) * CHUNK
            since = exponents_in[base : base + CHUNK, at]
            until = exponents_in[base + CHUNK : base + 2 * CHUNK, at]
            inner = dot((scores * scale).astype(bf16), v16)
            carried = dot_nt((q * scale * jnp.exp(since)).astype(bf16), state.astype(bf16))
            local_out[rows, at] = inner + carried
            from_start[rows, at] = (q * scale * jnp.exp(since + offset)).astype(bf16)
            total = since[CHUNK - 1 : CHUNK, :]
            state = state * jnp.exp(total) + dot_tn(v16, (k * jnp.exp(until)).astype(bf16))
            offset = offset + total
    acc[...] = jnp.zeros_like(acc)
    consumed[...] = jnp.zeros_like(consumed)
    for h in range(sq.shape[1] // head_size):
        stick_block(sq, pack, acc, consumed, h, head_size, True)


def merge(received, out_linear, out_stick, result):
    members = received.shape[0]
    half = out_linear.shape[0] // members
    lin = jnp.concatenate([received[j, :, :half] for j in range(members)], axis=1)
    stick = jnp.concatenate([received[j, :, half:] for j in range(members)], axis=1)
    result[...] = (dot(lin, out_linear[...]) + dot(stick, out_stick[...])).astype(bf16)


def finish(*refs, steps):
    position, local_out, from_start, gate, head_gain, sq, acc_in, consumed_in = refs[:8]
    packs, summaries = refs[8 : 8 + steps], refs[8 + steps : 8 + 2 * steps]
    merged, acc, consumed, state = refs[8 + 2 * steps :]
    head_size = head_gain.shape[1]
    here = position[0]
    acc[...] = acc_in[...]
    consumed[...] = consumed_in[...]
    state[...] = jnp.zeros_like(state)
    for r in range(1, steps + 1):

        @pl.when(r <= here)
        def _(pack=packs[r - 1]):
            for h in range(sq.shape[1] // head_size):
                stick_block(sq, pack, acc, consumed, h, head_size, False)

    for r in range(steps, 0, -1):

        @pl.when(r <= here)
        def _(one=summaries[r - 1]):
            tail = one[head_size:, :].astype(f32)
            kept = jnp.exp(tail[0:1, :] + tail[1:2, :])
            state[...] = state[...] * kept + one[:head_size, :].astype(f32)

    lin_cols = local_out.shape[1]
    for h in range(lin_cols // head_size):
        at = slice(h * head_size, (h + 1) * head_size)
        out = local_out[:, at] + dot_nt(from_start[:, at], state[:, at].astype(bf16))
        out = out * lax.rsqrt(jnp.mean(out * out, axis=1, keepdims=True) + norm_eps) * head_gain[...]
        g = gate[:, at].astype(f32)
        merged[:, at] = (out * (g / (1.0 + jnp.exp(-g)))).astype(bf16)
    merged[:, lin_cols:] = acc[...].astype(bf16)


def call(body, outs, count, scratch=(), flops=0, name=None):
    return pl.pallas_call(
        body,
        out_shape=outs,
        in_specs=count,
        out_specs=[VMEM] * len(outs),
        scratch_shapes=scratch,
        cost_estimate=pl.CostEstimate(flops=flops, bytes_accessed=1 << 22, transcendentals=1 << 20),
        name=name,
    )


def sent_back(array, axis):
    devices, here = lax.axis_size(axis), lax.axis_index(axis)
    if devices <= 8:
        return [
            lax.ppermute(array, axis, [(i, i + r) for i in range(devices - r)])
            for r in range(1, devices)
        ]
    everything = lax.all_gather(array, axis)
    return [
        lax.dynamic_index_in_dim(everything, (here - r) % devices, 0, keepdims=False)
        for r in range(1, devices)
    ]


def gathered(tokens):
    members = lax.axis_size("tp")
    groups = [list(range(parity, members, 2)) for parity in range(2)]
    same = lax.all_gather(tokens, "tp", axis_index_groups=groups)
    return same, lax.ppermute(same, "tp", [(i, i ^ 1) for i in range(members)])


def per_device(
    tokens, norm_gain, lin_query, lin_key, lin_value, lin_gate, gate_down, gate_up_weight,
    decay_offset_bias, lin_norm_gain, stick_query, stick_key, stick_value, key_bias,
    out_linear, out_stick,
):
    model_width = norm_gain.shape[0]
    head_size = lin_norm_gain.shape[0]
    count = tokens.shape[0]
    lin_cols, stick_cols = lin_query.shape[1], stick_query.shape[1]
    stick_heads = stick_cols // head_size
    shape = jax.ShapeDtypeStruct
    place = lax.axis_index("tp")[None].astype(jnp.int32)
    same, other = gathered(tokens)
    scaled, rescale, pack = call(
        project_first,
        [shape((count, model_width), bf16), shape((count, 1), f32),
         shape((2 * count + PAD, stick_cols), bf16)],
        [SMEM] + [VMEM] * 6, scratch=[pltpu.VMEM((1, model_width), f32)],
        flops=4 * count * model_width * stick_cols, name="first",
    )(place % 2, same, other, norm_gain, stick_key, stick_value, key_bias)
    packs = sent_back(pack, "sp")
    spans = jnp.asarray(span_matrices(), bf16)
    exponents, keys, values, summary = call(
        decay_state,
        [shape((spans.shape[0] * count // CHUNK, lin_cols), f32), shape((count, lin_cols), bf16),
         shape((count, lin_cols), bf16), shape((head_size + PAD, lin_cols), bf16)],
        [SMEM] + [VMEM] * 8, flops=1 << 31, name="state",
    )(place, scaled, rescale, lin_key, lin_value, gate_down.T, gate_up_weight,
      decay_offset_bias, spans)
    summaries = sent_back(summary, "sp")
    local_out, from_start, gate, sq, acc, consumed = call(
        project_rest,
        [shape((count, lin_cols), f32), shape((count, lin_cols), bf16),
         shape((count, lin_cols), bf16),
         shape((count, stick_cols), bf16), shape((count, stick_cols), f32),
         shape((count, stick_heads), f32)],
        [VMEM] * 9, flops=1 << 34, name="rest",
    )(scaled, rescale, stick_query, lin_query, lin_gate, exponents, keys, values, pack)
    steps = len(packs)
    (merged,) = call(
        functools.partial(finish, steps=steps),
        [shape((count, lin_cols + stick_cols), bf16)],
        [SMEM] + [VMEM] * (7 + 2 * steps),
        scratch=[pltpu.VMEM((count, stick_cols), f32), pltpu.VMEM((count, stick_heads), f32),
                 pltpu.VMEM((head_size, lin_cols), f32)],
        flops=1 << 32, name="finish",
    )(lax.axis_index("sp")[None].astype(jnp.int32), local_out, from_start, gate,
      lin_norm_gain[None], sq, acc, consumed, *packs, *summaries)
    members = lax.axis_size("tp")
    joined = lin_cols + stick_cols
    received = lax.all_to_all(
        merged.reshape(members, count // members, joined), "tp", split_axis=0, concat_axis=0, tiled=True
    )
    (result,) = call(
        merge, [shape((count // members, model_width), bf16)], [VMEM] * 3, flops=1 << 28, name="merge"
    )(received, out_linear, out_stick)
    return result


def solution(mesh):
    heads = P(None, "tp")
    placed = (
        P("sp", "tp"), P(), heads, heads, heads, heads, P(), P(), P("sp", "tp"), P(),
        heads, heads, heads, P("tp", "sp"), P(), P(),
    )
    return jax.shard_map(
        per_device, mesh=mesh, in_specs=placed, out_specs=P(("sp", "tp"), None), check_vma=False
    )
```

```python
import functools

import jax
import jax.numpy as jnp
import numpy as np
from jax import lax
from jax.experimental import pallas as pl
from jax.experimental.pallas import tpu as pltpu
from jax.sharding import PartitionSpec as P


norm_eps = 1e-06
gate_softness = 16.0
CHUNK = 128
PAD = 16
f32 = jnp.float32
bf16 = jnp.bfloat16
VMEM = pl.BlockSpec(memory_space=pltpu.VMEM)
SMEM = pl.BlockSpec(memory_space=pltpu.SMEM)


def dot(a, b):
    return jnp.dot(a, b, preferred_element_type=f32)


def dot_nt(a, b):
    return lax.dot_general(a, b, (((1,), (1,)), ((), ())), preferred_element_type=f32)


def dot_tn(a, b):
    return lax.dot_general(a, b, (((0,), (0,)), ((), ())), preferred_element_type=f32)


def split(x):
    hi = x.astype(bf16)
    return hi, (x - hi.astype(f32)).astype(bf16)


def halvings():
    size, result = CHUNK // 2, []
    while size:
        result.append(size)
        size //= 2
    return result


def span_matrices():
    t, i = np.arange(CHUNK)[:, None], np.arange(CHUNK)[None, :]
    parts = []
    for h in halvings():
        pivot = (t // (2 * h)) * 2 * h + h - 1
        parts.append(np.where(t > pivot, (i > pivot) & (i <= t), (i > t) & (i <= pivot)))
    parts.append(i <= t)
    parts.append(i > t)
    return np.concatenate(parts, 0).astype(np.float32)


def project_first(core, same, other, gain, wk, wv, bias, scaled, rescale, pack, wide_gain):
    pieces, count, width = same.shape
    wide_gain[...] = gain[...].astype(f32)[None]
    squares = jnp.zeros((count, 1), f32)
    for tokens, parity in ((same, core[0]), (other, 1 - core[0])):
        for j in range(pieces):
            at = pl.ds(pl.multiple_of((2 * j + parity) * width, CHUNK), width)
            part = tokens[j].astype(f32)
            squares = squares + jnp.sum(part * part, axis=1, keepdims=True)
            scaled[:, at] = (part * wide_gain[:, at]).astype(bf16)
    rescale[...] = lax.rsqrt(squares / scaled.shape[1] + norm_eps)
    both = dot(scaled[...], jnp.concatenate([wk[...], wv[...]], axis=1)) * rescale[...]
    cols = wk.shape[1]
    pack[:count, :] = both[:, :cols].astype(bf16)
    pack[count : 2 * count, :] = both[:, cols:].astype(bf16)
    extra = pack.shape[0] - 2 * count
    heads = bias.shape[0]
    head_size = cols // heads
    row = lax.broadcasted_iota(jnp.int32, (extra, head_size), 0)
    for h in range(heads):
        block = jnp.zeros((extra, head_size), f32)
        for m in range(count // head_size):
            piece = bias[h : h + 1, m * head_size : (m + 1) * head_size].astype(f32)
            block = jnp.where(row == m, piece, block)
        pack[2 * count :, h * head_size : (h + 1) * head_size] = block.astype(bf16)


def stick_block(query, pack, acc, consumed, head, head_size, own):
    count = query.shape[0]
    cols = pl.ds(head * head_size, head_size)
    j = lax.broadcasted_iota(jnp.int32, (2 * CHUNK, CHUNK), 0) % CHUNK
    s = lax.broadcasted_iota(jnp.int32, (2 * CHUNK, CHUNK), 1)
    later = (j >= s).astype(bf16)
    for m in reversed(range(count // CHUNK)):
        first = m * CHUNK if own else 0
        rows = pl.ds(first, count - first)
        keys = pack[pl.ds(m * CHUNK, CHUNK), cols]
        values = pack[pl.ds(count + m * CHUNK, CHUNK), cols]
        bias = pack[pl.ds(2 * count, PAD), cols][m : m + 1, :].astype(f32)
        z = dot_nt(query[rows, cols], keys) * head_size ** (-0.5) + bias
        falling = -(jnp.maximum(z, 0.0) + jnp.log(1.0 + jnp.exp(-jnp.abs(z))))
        if own:
            t = lax.broadcasted_iota(jnp.int32, z.shape, 0)
            visible = lax.broadcasted_iota(jnp.int32, z.shape, 1) < t
            falling = jnp.where(visible, falling, 0.0)
        sums = dot(jnp.concatenate(split(falling), axis=1), later)
        before = consumed[rows, pl.ds(head, 1)]
        shares = jnp.exp(z + sums + before)
        if own:
            shares = jnp.where(visible, shares, 0.0)
        acc[rows, cols] += dot(shares.astype(bf16), values)
        consumed[rows, pl.ds(head, 1)] = before + sums[:, 0:1]


def project_rest(
    place, scaled, rescale, wsq, wq, wk, wv, wg, down, up, bias, pack, spans,
    local_out, from_start, gate, summary, sq, acc, consumed,
):
    cols = wq.shape[1]
    head_size = CHUNK
    count = scaled.shape[0]
    scale = head_size ** (-0.5)
    inv = rescale[...]
    x = scaled[...]
    low = (dot_nt(x, down[...]) * inv).astype(bf16)
    own = pl.ds(pl.multiple_of(place[0] * cols, CHUNK), cols)
    pre = dot(low, up[:, own]) + bias[...]
    decay = (jnp.minimum(pre, 0.0) - jnp.log(1.0 + jnp.exp(-jnp.abs(pre)))) / gate_softness
    qk = dot(x, jnp.concatenate([wq[...], wk[...]], axis=1)) * inv
    vg = dot(x, jnp.concatenate([wv[...], wg[...]], axis=1)) * inv
    gate[...] = vg[:, cols:].astype(bf16)
    sq[...] = (dot(x, wsq[...]) * inv).astype(bf16)
    t = lax.broadcasted_iota(jnp.int32, (CHUNK, CHUNK), 0)
    s = lax.broadcasted_iota(jnp.int32, (CHUNK, CHUNK), 1)
    sizes = halvings()
    for h in range(cols // head_size):
        at = slice(h * head_size, (h + 1) * head_size)
        state = jnp.zeros((head_size, head_size), f32)
        offset = jnp.zeros((1, head_size), f32)
        for n in range(count // CHUNK):
            rows = slice(n * CHUNK, (n + 1) * CHUNK)
            q16 = qk[rows, h * head_size : (h + 1) * head_size].astype(bf16)
            k16 = qk[rows, cols + h * head_size : cols + (h + 1) * head_size].astype(bf16)
            v16 = vg[rows, at].astype(bf16)
            q, k = q16.astype(f32), k16.astype(f32)
            both = dot(spans[...], jnp.concatenate(split(decay[rows, at]), axis=1))
            exponents = both[:, :head_size] + both[:, head_size:]
            scores = jnp.where(t == s, dot_nt(q16, k16), 0.0)
            for level, size in enumerate(sizes):
                e = jnp.exp(exponents[level * CHUNK : (level + 1) * CHUNK])
                part = dot_nt((q * e).astype(bf16), (k * e).astype(bf16))
                ok = (t // (2 * size) == s // (2 * size)) & (t % (2 * size) >= size)
                scores = jnp.where(ok & (s % (2 * size) < size), part, scores)
            since = exponents[len(sizes) * CHUNK : (len(sizes) + 1) * CHUNK]
            until = exponents[(len(sizes) + 1) * CHUNK :]
            inner = dot((scores * scale).astype(bf16), v16)
            carried = dot_nt((q * scale * jnp.exp(since)).astype(bf16), state.astype(bf16))
            local_out[rows, at] = inner + carried
            from_start[rows, at] = (q * scale * jnp.exp(since + offset)).astype(bf16)
            total = since[CHUNK - 1 : CHUNK, :]
            state = state * jnp.exp(total) + dot_tn(v16, (k * jnp.exp(until)).astype(bf16))
            offset = offset + total
        summary[:head_size, at] = state.astype(bf16)
        row = lax.broadcasted_iota(jnp.int32, (PAD, head_size), 0)
        high, rest = split(offset)
        tail = jnp.where(row == 0, high.astype(f32), jnp.where(row == 1, rest.astype(f32), 0.0))
        summary[head_size:, at] = tail.astype(bf16)
    acc[...] = jnp.zeros_like(acc)
    consumed[...] = jnp.zeros_like(consumed)
    for h in range(sq.shape[1] // head_size):
        stick_block(sq, pack, acc, consumed, h, head_size, True)


def merge(received, out_linear, out_stick, result):
    members = received.shape[0]
    half = out_linear.shape[0] // members
    lin = jnp.concatenate([received[j, :, :half] for j in range(members)], axis=1)
    stick = jnp.concatenate([received[j, :, half:] for j in range(members)], axis=1)
    result[...] = (dot(lin, out_linear[...]) + dot(stick, out_stick[...])).astype(bf16)


def finish(*refs, steps):
    position, local_out, from_start, gate, head_gain, sq, acc_in, consumed_in = refs[:8]
    packs, summaries = refs[8 : 8 + steps], refs[8 + steps : 8 + 2 * steps]
    merged, acc, consumed, state = refs[8 + 2 * steps :]
    head_size = head_gain.shape[1]
    here = position[0]
    acc[...] = acc_in[...]
    consumed[...] = consumed_in[...]
    state[...] = jnp.zeros_like(state)
    for r in range(1, steps + 1):

        @pl.when(r <= here)
        def _(pack=packs[r - 1]):
            for h in range(sq.shape[1] // head_size):
                stick_block(sq, pack, acc, consumed, h, head_size, False)

    for r in range(steps, 0, -1):

        @pl.when(r <= here)
        def _(one=summaries[r - 1]):
            tail = one[head_size:, :].astype(f32)
            kept = jnp.exp(tail[0:1, :] + tail[1:2, :])
            state[...] = state[...] * kept + one[:head_size, :].astype(f32)

    lin_cols = local_out.shape[1]
    for h in range(lin_cols // head_size):
        at = slice(h * head_size, (h + 1) * head_size)
        out = local_out[:, at] + dot_nt(from_start[:, at], state[:, at].astype(bf16))
        out = out * lax.rsqrt(jnp.mean(out * out, axis=1, keepdims=True) + norm_eps) * head_gain[...]
        g = gate[:, at].astype(f32)
        merged[:, at] = (out * (g / (1.0 + jnp.exp(-g)))).astype(bf16)
    merged[:, lin_cols:] = acc[...].astype(bf16)


def call(body, outs, count, scratch=(), flops=0, name=None):
    return pl.pallas_call(
        body,
        out_shape=outs,
        in_specs=count,
        out_specs=[VMEM] * len(outs),
        scratch_shapes=scratch,
        cost_estimate=pl.CostEstimate(flops=flops, bytes_accessed=1 << 22, transcendentals=1 << 20),
        name=name,
    )


def sent_back(array, axis):
    devices, here = lax.axis_size(axis), lax.axis_index(axis)
    if devices <= 8:
        return [
            lax.ppermute(array, axis, [(i, i + r) for i in range(devices - r)])
            for r in range(1, devices)
        ]
    everything = lax.all_gather(array, axis)
    return [
        lax.dynamic_index_in_dim(everything, (here - r) % devices, 0, keepdims=False)
        for r in range(1, devices)
    ]


def gathered(tokens):
    members = lax.axis_size("tp")
    groups = [list(range(parity, members, 2)) for parity in range(2)]
    same = lax.all_gather(tokens, "tp", axis_index_groups=groups)
    return same, lax.ppermute(same, "tp", [(i, i ^ 1) for i in range(members)])


def per_device(
    tokens, norm_gain, lin_query, lin_key, lin_value, lin_gate, gate_down, gate_up_weight,
    decay_offset_bias, lin_norm_gain, stick_query, stick_key, stick_value, key_bias,
    out_linear, out_stick,
):
    model_width = norm_gain.shape[0]
    head_size = lin_norm_gain.shape[0]
    count = tokens.shape[0]
    lin_cols, stick_cols = lin_query.shape[1], stick_query.shape[1]
    stick_heads = stick_cols // head_size
    shape = jax.ShapeDtypeStruct
    place = lax.axis_index("tp")[None].astype(jnp.int32)
    same, other = gathered(tokens)
    scaled, rescale, pack = call(
        project_first,
        [shape((count, model_width), bf16), shape((count, 1), f32),
         shape((2 * count + PAD, stick_cols), bf16)],
        [SMEM] + [VMEM] * 6, scratch=[pltpu.VMEM((1, model_width), f32)],
        flops=4 * count * model_width * stick_cols, name="first",
    )(place % 2, same, other, norm_gain, stick_key, stick_value, key_bias)
    packs = sent_back(pack, "sp")
    local_out, from_start, gate, summary, sq, acc, consumed = call(
        project_rest,
        [shape((count, lin_cols), f32), shape((count, lin_cols), bf16),
         shape((count, lin_cols), bf16), shape((head_size + PAD, lin_cols), bf16),
         shape((count, stick_cols), bf16), shape((count, stick_cols), f32),
         shape((count, stick_heads), f32)],
        [SMEM] + [VMEM] * 12, flops=1 << 34, name="rest",
    )(place, scaled, rescale, stick_query, lin_query, lin_key, lin_value, lin_gate, gate_down.T,
      gate_up_weight, decay_offset_bias, pack, jnp.asarray(span_matrices(), bf16))
    summaries = sent_back(summary, "sp")
    steps = len(packs)
    (merged,) = call(
        functools.partial(finish, steps=steps),
        [shape((count, lin_cols + stick_cols), bf16)],
        [SMEM] + [VMEM] * (7 + 2 * steps),
        scratch=[pltpu.VMEM((count, stick_cols), f32), pltpu.VMEM((count, stick_heads), f32),
                 pltpu.VMEM((head_size, lin_cols), f32)],
        flops=1 << 32, name="finish",
    )(lax.axis_index("sp")[None].astype(jnp.int32), local_out, from_start, gate,
      lin_norm_gain[None], sq, acc, consumed, *packs, *summaries)
    members = lax.axis_size("tp")
    joined = lin_cols + stick_cols
    received = lax.all_to_all(
        merged.reshape(members, count // members, joined), "tp", split_axis=0, concat_axis=0, tiled=True
    )
    tile = model_width // 4
    heads_rows, stick_rows = out_linear.shape[0], out_stick.shape[0]
    rows = count // members
    return pl.pallas_call(
        merge,
        grid=(model_width // tile,),
        out_shape=shape((rows, model_width), bf16),
        in_specs=[
            pl.BlockSpec(received.shape, lambda n: (0, 0, 0)),
            pl.BlockSpec((heads_rows, tile), lambda n: (0, n)),
            pl.BlockSpec((stick_rows, tile), lambda n: (0, n)),
        ],
        out_specs=pl.BlockSpec((rows, tile), lambda n: (0, n)),
        name="merge",
    )(received, out_linear, out_stick)


def solution(mesh):
    heads = P(None, "tp")
    placed = (
        P("sp", "tp"), P(), heads, heads, heads, heads, P(), P(), P("sp", "tp"), P(),
        heads, heads, heads, P("tp", "sp"), P(), P(),
    )
    return jax.shard_map(
        per_device, mesh=mesh, in_specs=placed, out_specs=P(("sp", "tp"), None), check_vma=False
    )
```
